512 devices in a mesh: grp: 2 (over y), sp: 32 (over z, core), tp: 8 (over x).
Axes of the slice: x: 8, y: 2, z: 16, core: 2. Of those that a mesh axis runs over, the one named last changes fastest.
The devices are a block of a 8x8x16 slice.
Arguments:
- tokens: bfloat16 [32768, 2048], P(('grp', 'sp'), 'tp'), parts along dimension 0, may hold values from -140 to 140, as said below
- mix_gain: bfloat16 [2, 2048], replicated, may hold values from 0.099609375 to 1.8984375
- gate_weight: bfloat16 [2, 2048, 2048], P(None, 'sp', 'tp'), may hold values from -0.125 to 0.125
- mix_weight: bfloat16 [2, 2048, 2048], P(None, 'sp', 'tp'), may hold values from -0.125 to 0.125
- value_weight: bfloat16 [2, 2048, 2048], P(None, 'sp', 'tp'), may hold values from -0.125 to 0.125
- out_weight: bfloat16 [2, 2048, 2048], P(None, 'sp', 'tp'), may hold values from -0.125 to 0.125
- conv_taps: bfloat16 [2, 3, 2048], P(None, None, 'tp'), may hold values from -3.5 to 3.5
Outputs:
- result_stream: bfloat16 [32768, 2048], P(('grp', 'sp'), 'tp'), parts along dimension 0
The draws below stay inside these ranges and needn't reach their ends.
There are 2 independent parts, one for each index of `grp`. The reference program is written for one: setup_inputs(seed, part) draws one part's arguments, and reference() takes and returns one part's arrays. A program takes and returns all parts, laid end to end along the dimension named above; an argument that names none is the same for every part. Nothing has to cross between parts.
Inputs may be any that keep to these rules, and one draw needn't show every extreme that they name: `tokens`: activations with feature scales of several sizes.
All inputs are finite; a program needn't handle non-finite values.
Results may differ from the reference program's by a relative error of at most 0.015.
Values may be sent and summed in bfloat16 or wider, within the bound.
No kernel may reach another device: no remote copies, remote signals or barrier semaphores. Data moves between devices by JAX's collectives and lax.ppermute only.
A program may use at most 64 MiB of HBM per device.

```python
import jax
import jax.numpy as jnp
from jax import lax

D = 2048
TAPS = 3
LAYERS = 2
TOKENS = 16384


def draw_tokens(key, part):
    subkeys = jax.random.split(key, 2)
    normal_part = jnp.clip(jax.random.normal(subkeys[0], (TOKENS, D), jnp.float32), -6.0, 6.0)
    column = 10.0 ** (jax.random.uniform(subkeys[1], (D,), jnp.float32) - 0.5)
    column = column * 3.0 ** (jnp.arange(D, dtype=jnp.float32) / D - 0.5)
    return (normal_part * column).astype(jnp.bfloat16)


def levels(rng, shape, cuts, least, top_value):
    gain, own = 1.0, jax.random.fold_in(rng, 6)
    for position, parts in cuts:
        draws = jnp.exp(jax.random.uniform(jax.random.fold_in(own, position), (parts,), jnp.float32, least / len(cuts), top_value / len(cuts)))
        gain = gain * jnp.repeat(draws, shape[position] // parts).reshape([-1 if axis == position else 1 for axis in range(len(shape))])
    return gain


def scatter_about(own_key, shape, scale, reach, pieces=(), kind=jnp.bfloat16):
    entries = jax.random.normal(own_key, shape, jnp.float32) * scale
    if len(pieces) > 0:
        entries = levels(own_key, shape, pieces, -0.22, 0.18) * entries
    return jnp.clip(entries, min=-reach, max=reach).astype(kind)


def setup_inputs(seed: int = 0, part: int = 0) -> dict:
    arg_keys = jax.random.split(jax.random.key(seed), 8)
    own_keys = jax.random.split(jax.random.fold_in(arg_keys[7], part), 8)
    tokens = draw_tokens(jax.random.fold_in(jax.random.fold_in(arg_keys[7], part), 71), part)
    mix_gain = jnp.clip(1.0 + 0.18 * jax.random.normal(arg_keys[1], (LAYERS, D), jnp.float32), 0.099609375, 1.8984375).astype(jnp.bfloat16)
    gate_weight = scatter_about(arg_keys[2], (LAYERS, D, D), D ** -0.5, 0.125, ((1, 32), (2, 8)))
    mix_weight = scatter_about(arg_keys[3], (LAYERS, D, D), D ** -0.5, 0.125, ((1, 32), (2, 8)))
    value_weight = scatter_about(arg_keys[4], (LAYERS, D, D), D ** -0.5, 0.125, ((1, 32), (2, 8)))
    out_weight = scatter_about(arg_keys[5], (LAYERS, D, D), D ** -0.5, 0.125, ((1, 32), (2, 8)))
    conv_taps = scatter_about(arg_keys[6], (LAYERS, TAPS, D), TAPS ** -0.5, 3.5, ((2, 8),))
    return {"tokens": tokens, "mix_gain": mix_gain, "gate_weight": gate_weight, "mix_weight": mix_weight, "value_weight": value_weight, "out_weight": out_weight, "conv_taps": conv_taps}


EPS = 1e-06

def reference(tokens, mix_gain, gate_weight, mix_weight, value_weight, out_weight, conv_taps):
    stream = tokens
    for layer_index in range(LAYERS):
        wide_rows = stream.astype(jnp.float32)
        factor = lax.rsqrt(lax.optimization_barrier(jnp.mean(wide_rows * wide_rows, axis=1, keepdims=True)) + EPS)
        normed = (wide_rows * factor * mix_gain[layer_index].astype(jnp.float32)).astype(jnp.bfloat16)
        gate = jnp.dot(normed, gate_weight[layer_index], preferred_element_type=jnp.float32).astype(jnp.bfloat16)
        inner = jnp.dot(normed, mix_weight[layer_index], preferred_element_type=jnp.float32).astype(jnp.bfloat16)
        values = jnp.dot(normed, value_weight[layer_index], preferred_element_type=jnp.float32).astype(jnp.bfloat16)
        carried = inner.astype(jnp.float32) * values.astype(jnp.float32)
        padded = jnp.pad(carried, ((TAPS - 1, 0), (0, 0)))
        row_count = carried.shape[0]
        tap_rows = conv_taps[layer_index].astype(jnp.float32)
        conv = jnp.zeros_like(carried)
        for tap_index in range(TAPS):
            conv = conv + tap_rows[tap_index] * padded[tap_index:tap_index + row_count]
        mixed = (gate.astype(jnp.float32) * conv).astype(jnp.bfloat16)
        product = jnp.dot(mixed, out_weight[layer_index], preferred_element_type=jnp.float32)
        stream = (wide_rows + product).astype(jnp.bfloat16)
    return stream
```

```python
import jax
import jax.numpy as jnp
from jax import lax
from jax.sharding import PartitionSpec as P

EPS = 1e-06
TILE_ROWS = 8
F32 = jnp.float32
BF16 = jnp.bfloat16


def passed_along(x, axis, by):
    devices = lax.axis_size(axis)
    pairs = [(i, i + by) for i in range(devices) if 0 <= i + by < devices]
    return lax.ppermute(x, axis, pairs)


def turned(x, axis, by):
    devices = lax.axis_size(axis)
    return lax.ppermute(x, axis, [(i, (i + by) % devices) for i in range(devices)])


def ring(block, axis):
    devices = lax.axis_size(axis)
    arrived = [(0, block)]
    up = down = block
    for step in range(1, (devices - 1) // 2 + 1):
        up, down = turned(up, axis, 1), turned(down, axis, -1)
        arrived += [(-step, up), (step, down)]
    if devices % 2 == 0:
        half = block.shape[0] // 16 * 8
        up, down = turned(up[:half], axis, 1), turned(down[half:], axis, -1)
        arrived.append((devices // 2, jnp.concatenate([up, down], axis=0)))
    return arrived


def rows_of(weight, owner, count):
    return lax.dynamic_slice_in_dim(weight, owner * count, count, axis=0)


def convolve(carried, tap_rows):
    reach = tap_rows.shape[0] - 1
    count = carried.shape[0]
    padded = jnp.concatenate([jnp.zeros((reach, carried.shape[1]), F32), carried], axis=0)
    result = jnp.zeros_like(carried)
    for tap in range(reach + 1):
        result = result + tap_rows[tap].astype(F32) * padded[tap : tap + count]
    return result


def shards(tokens, mix_gain, gate_weight, mix_weight, value_weight, out_weight, conv_taps):
    layers, _, width = gate_weight.shape
    devices = lax.axis_size("tp")
    me = lax.axis_index("tp")
    reach = conv_taps.shape[1] - 1
    fringe = -(-reach * layers // TILE_ROWS) * TILE_ROWS
    before = passed_along(tokens[tokens.shape[0] - fringe :], "sp", 1)
    stream = jnp.concatenate([before, tokens], axis=0)

    mine = jnp.concatenate(
        [w[l] for l in range(layers) for w in (gate_weight, mix_weight, value_weight, out_weight)], axis=0
    ).reshape(layers * 4, -1, width)
    whole = lax.all_gather(mine, "sp", axis=1, tiled=True)

    for l in range(layers):
        gains = mix_gain[l].reshape(devices, 1, width)
        total = [None] * 3
        squares = 0.0
        for offset, block in ring(stream, "tp"):
            owner = lax.rem(me + offset + devices, devices)
            wide = block.astype(F32)
            squares = squares + jnp.sum(wide * wide, axis=1, keepdims=True)
            scaled = (wide * lax.dynamic_index_in_dim(gains, owner, 0, False).astype(F32)).astype(BF16)
            for k in range(3):
                part = jnp.dot(scaled, rows_of(whole[4 * l + k], owner, width), preferred_element_type=F32)
                total[k] = part if total[k] is None else total[k] + part
        factor = lax.rsqrt(squares / (devices * width) + EPS)
        gate, inner, values = ((t * factor).astype(BF16).astype(F32) for t in total)
        mixed = (gate * convolve(inner * values, conv_taps[l])).astype(BF16)
        product = stream.astype(F32)
        for offset, block in ring(mixed, "tp"):
            owner = lax.rem(me + offset + devices, devices)
            product = product + jnp.dot(block, rows_of(whole[4 * l + 3], owner, width), preferred_element_type=F32)
        stream = product.astype(BF16)
    return stream[fringe:]


def solution(mesh):
    return jax.shard_map(
        shards,
        mesh=mesh,
        in_specs=(
            P(("grp", "sp"), "tp"),
            P(),
            P(None, "sp", "tp"),
            P(None, "sp", "tp"),
            P(None, "sp", "tp"),
            P(None, "sp", "tp"),
            P(None, None, "tp"),
        ),
        out_specs=P(("grp", "sp"), "tp"),
        check_vma=False,
    )
```

```python
import jax
import jax.numpy as jnp
from jax import lax
from jax.sharding import PartitionSpec as P

EPS = 1e-06
TILE_ROWS = 8
CHUNKS = 2
F32 = jnp.float32
BF16 = jnp.bfloat16


def passed_along(x, axis, by):
    devices = lax.axis_size(axis)
    pairs = [(i, i + by) for i in range(devices) if 0 <= i + by < devices]
    return lax.ppermute(x, axis, pairs)


def swapped(x, step):
    lines, devices = lax.axis_size("sp"), lax.axis_size("tp")
    pairs = []
    for s in range(lines):
        for i in range(devices):
            to = i + 1 if i % 2 == (step + s) % 2 else i - 1
            pairs.append((s * devices + i, s * devices + to % devices))
    return lax.ppermute(x, ("sp", "tp"), pairs)


def arriving(block):
    devices = lax.axis_size("tp")
    me, line = lax.axis_index("tp"), lax.axis_index("sp")
    side = jnp.where(me % 2 == line % 2, 1, -1)
    rows = block.shape[0]

    def owner(k):
        return (me + k * side + devices) % devices

    pair = jnp.concatenate([block, swapped(block, 0)], axis=0)
    blocks = [(owner(0), pair[:rows]), (owner(1), pair[rows:])]
    for step in range(1, devices // 2):
        pair = swapped(pair, step)
        near = -step if step % 2 else step
        far = near - 1 if step % 2 else near + 1
        blocks += [(owner(near), pair[:rows]), (owner(far), pair[rows:])]
    return blocks


def rows_of(weight, owner, count):
    return lax.dynamic_slice_in_dim(weight, owner * count, count, axis=0)


def convolve(carried, tap_rows):
    reach = tap_rows.shape[0] - 1
    count = carried.shape[0]
    padded = jnp.concatenate([jnp.zeros((reach, carried.shape[1]), F32), carried], axis=0)
    result = jnp.zeros_like(carried)
    for tap in range(reach + 1):
        result = result + tap_rows[tap].astype(F32) * padded[tap : tap + count]
    return result


def shards(tokens, mix_gain, gate_weight, mix_weight, value_weight, out_weight, conv_taps):
    layers, _, width = gate_weight.shape
    devices = lax.axis_size("tp")
    reach = conv_taps.shape[1] - 1
    fringe = -(-reach * layers // TILE_ROWS) * TILE_ROWS
    before = passed_along(tokens[tokens.shape[0] - fringe :], "sp", 1)
    extended = jnp.concatenate([before, tokens], axis=0)
    count = tokens.shape[0] // CHUNKS
    streams = [extended[c * count : (c + 1) * count + fringe] for c in range(CHUNKS)]
    kinds = (gate_weight, mix_weight, value_weight, out_weight)
    whole = lax.all_gather(jnp.concatenate(kinds, axis=0), "sp", axis=1, tiled=True)

    for l in range(layers):
        gains = mix_gain[l].reshape(devices, 1, width)
        for c in range(CHUNKS):
            stream = streams[c]
            total = [0.0] * 3
            squares = 0.0
            for owner, block in arriving(stream):
                wide = block.astype(F32)
                squares = squares + jnp.sum(wide * wide, axis=1, keepdims=True)
                scaled = (wide * lax.dynamic_index_in_dim(gains, owner, 0, False).astype(F32)).astype(BF16)
                for k in range(3):
                    part = rows_of(whole[k * layers + l], owner, width)
                    total[k] = total[k] + jnp.dot(scaled, part, preferred_element_type=F32)
            factor = lax.rsqrt(squares / (devices * width) + EPS)
            gate, inner, values = ((t * factor).astype(BF16).astype(F32) for t in total)
            mixed = (gate * convolve(inner * values, conv_taps[l])).astype(BF16)
            product = stream.astype(F32)
            for owner, block in arriving(mixed):
                part = rows_of(whole[3 * layers + l], owner, width)
                product = product + jnp.dot(block, part, preferred_element_type=F32)
            streams[c] = product.astype(BF16)
    return jnp.concatenate([stream[fringe:] for stream in streams], axis=0)


def solution(mesh):
    return jax.shard_map(
        shards,
        mesh=mesh,
        in_specs=(
            P(("grp", "sp"), "tp"),
            P(),
            P(None, "sp", "tp"),
            P(None, "sp", "tp"),
            P(None, "sp", "tp"),
            P(None, "sp", "tp"),
            P(None, None, "tp"),
        ),
        out_specs=P(("grp", "sp"), "tp"),
        check_vma=False,
    )
```

```python
import jax
import jax.numpy as jnp
from jax import lax
from jax.sharding import PartitionSpec as P

EPS = 1e-06
TILE_ROWS = 8
CHUNKS = 2
F32 = jnp.float32
BF16 = jnp.bfloat16


def passed_along(x, axis, by):
    devices = lax.axis_size(axis)
    pairs = [(i, i + by) for i in range(devices) if 0 <= i + by < devices]
    return lax.ppermute(x, axis, pairs)


def turned(x, axis, by):
    devices = lax.axis_size(axis)
    return lax.ppermute(x, axis, [(i, (i + by) % devices) for i in range(devices)])


def whole_rows(block, axis):
    devices = lax.axis_size(axis)
    arrived = {0: block}
    up = down = block
    for step in range(1, (devices - 1) // 2 + 1):
        up, down = turned(up, axis, 1), turned(down, axis, -1)
        arrived[-step], arrived[step] = up, down
    if devices % 2 == 0:
        later, up = lax.optimization_barrier((block, up))
        arrived[-step] = up
        arrived[devices // 2] = turned(later, axis, devices // 2)
    offsets = sorted(arrived)
    twice = jnp.concatenate([arrived[k] for k in offsets] * 2, axis=1)
    width = block.shape[1]
    first = (lax.axis_index(axis) + offsets[0] + devices) % devices
    return lax.dynamic_slice_in_dim(twice, (devices - first) % devices * width, devices * width, axis=1)


def side_by_side(shard, axis):
    devices = lax.axis_size(axis)
    copies = jnp.broadcast_to(shard, (devices, *shard.shape))
    pieces = lax.all_to_all(copies, axis, split_axis=0, concat_axis=0, tiled=True)
    return jnp.concatenate([pieces[i] for i in range(devices)], axis=1)


def summed(x, axis):
    devices = lax.axis_size(axis)
    count = -(-x.shape[0] // 128) * 128
    copies = jnp.broadcast_to(jnp.pad(x, (0, count - x.shape[0])).reshape(-1, 128), (devices, count // 128, 128))
    return jnp.sum(lax.all_to_all(copies, axis, split_axis=0, concat_axis=0, tiled=True), axis=0).reshape(-1)[: x.shape[0]]


def swapped(x, step):
    lines, devices = lax.axis_size("sp"), lax.axis_size("tp")
    pairs = []
    for s in range(lines):
        for i in range(devices):
            to = i + 1 if i % 2 == (step + s) % 2 else i - 1
            pairs.append((s * devices + i, s * devices + to % devices))
    return lax.ppermute(x, ("sp", "tp"), pairs)


def arriving(block):
    devices = lax.axis_size("tp")
    me, line = lax.axis_index("tp"), lax.axis_index("sp")
    side = jnp.where(me % 2 == line % 2, 1, -1)
    rows = block.shape[0]

    def owner(k):
        return (me + k * side + devices) % devices

    pair = jnp.concatenate([block, swapped(block, 0)], axis=0)
    blocks = [(owner(0), pair[:rows]), (owner(1), pair[rows:])]
    for step in range(1, devices // 2):
        pair = swapped(pair, step)
        near = -step if step % 2 else step
        far = near - 1 if step % 2 else near + 1
        blocks += [(owner(near), pair[:rows]), (owner(far), pair[rows:])]
    return blocks


def product(a, b):
    return jnp.dot(a, b, preferred_element_type=F32)


def convolve(carried, tap_rows):
    reach = tap_rows.shape[0] - 1
    count = carried.shape[0]
    padded = jnp.concatenate([jnp.zeros((reach, carried.shape[1]), F32), carried], axis=0)
    result = jnp.zeros_like(carried)
    for tap in range(reach + 1):
        result = result + tap_rows[tap].astype(F32) * padded[tap : tap + count]
    return result


def gated(projected, tap_rows):
    gate, inner, values = (p.astype(BF16).astype(F32) for p in projected)
    return (gate * convolve(inner * values, tap_rows)).astype(BF16)


def factor_of(squares, count):
    return lax.rsqrt(squares / count + EPS)


def shards(tokens, mix_gain, gate_weight, mix_weight, value_weight, out_weight, conv_taps):
    _, _, width = gate_weight.shape
    features = mix_gain.shape[1]
    reach = conv_taps.shape[1] - 1
    fringe = -(-reach * 2 // TILE_ROWS) * TILE_ROWS
    inward = (gate_weight, mix_weight, value_weight)
    mine = jnp.concatenate([*inward, out_weight[:1]], axis=0)
    early = lax.all_gather(mine, "sp", axis=1, tiled=True)

    before = passed_along(tokens[tokens.shape[0] - fringe :], "sp", 1)
    stream = jnp.concatenate([before, tokens], axis=0)
    whole = whole_rows(stream, "tp").astype(F32)
    factor = factor_of(jnp.sum(whole * whole, axis=1, keepdims=True), features)
    normed = (whole * factor * mix_gain[0].astype(F32)).astype(BF16)
    scaled = (whole * mix_gain[1].astype(F32)).astype(BF16)

    shared = side_by_side(out_weight[0], "tp")
    shared, normed, scaled = lax.optimization_barrier((shared, normed, scaled))
    out_rows = (shared.astype(F32) * mix_gain[1].astype(F32)).astype(BF16)
    through = [product(out_rows, early[2 * k + 1]).astype(BF16) for k in range(3)]
    late = lax.all_gather(jnp.stack([*through, out_weight[1]]), "sp", axis=1, tiled=True)

    mixed = gated([product(normed, early[2 * k]) for k in range(3)], conv_taps[0])
    straight = [product(scaled, early[2 * k + 1]) for k in range(3)]
    all_mixed, *straight = lax.optimization_barrier((whole_rows(mixed, "tp"), *straight))
    stream = (stream.astype(F32) + product(all_mixed, early[6])).astype(BF16)
    wide = stream.astype(F32)
    squares = summed(jnp.sum(wide * wide, axis=1), "tp")
    factor = factor_of(squares, features)[:, None]

    mixed = gated([(straight[k] + product(all_mixed, late[k])) * factor for k in range(3)], conv_taps[1])
    results = []
    count = tokens.shape[0] // CHUNKS
    for c in range(CHUNKS):
        part = slice(fringe + c * count, fringe + (c + 1) * count)
        total = stream[part].astype(F32)
        for owner, block in arriving(mixed[part]):
            total = total + product(block, lax.dynamic_slice_in_dim(late[3], owner * width, width, axis=0))
        results.append(total.astype(BF16))
    return jnp.concatenate(results, axis=0)


def solution(mesh):
    return jax.shard_map(
        shards,
        mesh=mesh,
        in_specs=(
            P(("grp", "sp"), "tp"),
            P(),
            P(None, "sp", "tp"),
            P(None, "sp", "tp"),
            P(None, "sp", "tp"),
            P(None, "sp", "tp"),
            P(None, None, "tp"),
        ),
        out_specs=P(("grp", "sp"), "tp"),
        check_vma=False,
    )
```

```python
import jax
import jax.numpy as jnp
from jax import lax
from jax.experimental import pallas as pl
from jax.sharding import PartitionSpec as P

EPS = 1e-06
TILE_ROWS = 8
CHUNKS = 2
F32 = jnp.float32
BF16 = jnp.bfloat16


def passed_along(x, axis, by):
    devices = lax.axis_size(axis)
    pairs = [(i, i + by) for i in range(devices) if 0 <= i + by < devices]
    return lax.ppermute(x, axis, pairs)


def turned(x, axis, by):
    devices = lax.axis_size(axis)
    return lax.ppermute(x, axis, [(i, (i + by) % devices) for i in range(devices)])


def whole_rows(block, axis):
    devices = lax.axis_size(axis)
    arrived = {0: block}
    up = down = block
    for step in range(1, (devices - 1) // 2 + 1):
        up, down = turned(up, axis, 1), turned(down, axis, -1)
        arrived[-step], arrived[step] = up, down
    if devices % 2 == 0:
        later, up = lax.optimization_barrier((block, up))
        arrived[-step] = up
        arrived[devices // 2] = turned(later, axis, devices // 2)
    offsets = sorted(arrived)
    twice = jnp.concatenate([arrived[k] for k in offsets] * 2, axis=1)
    width = block.shape[1]
    first = (lax.axis_index(axis) + offsets[0] + devices) % devices
    return lax.dynamic_slice_in_dim(twice, (devices - first) % devices * width, devices * width, axis=1)


def side_by_side(shard, axis):
    devices = lax.axis_size(axis)
    copies = jnp.broadcast_to(shard, (devices, *shard.shape))
    pieces = lax.all_to_all(copies, axis, split_axis=0, concat_axis=0, tiled=True)
    return jnp.concatenate([pieces[i] for i in range(devices)], axis=1)


def summed(x, axis):
    devices = lax.axis_size(axis)
    count = -(-x.shape[0] // 128) * 128
    copies = jnp.broadcast_to(jnp.pad(x, (0, count - x.shape[0])).reshape(-1, 128), (devices, count // 128, 128))
    return jnp.sum(lax.all_to_all(copies, axis, split_axis=0, concat_axis=0, tiled=True), axis=0).reshape(-1)[: x.shape[0]]


def swapped(x, step):
    lines, devices = lax.axis_size("sp"), lax.axis_size("tp")
    pairs = []
    for s in range(lines):
        for i in range(devices):
            to = i + 1 if i % 2 == (step + s) % 2 else i - 1
            pairs.append((s * devices + i, s * devices + to % devices))
    return lax.ppermute(x, ("sp", "tp"), pairs)


def arriving(block):
    devices = lax.axis_size("tp")
    me, line = lax.axis_index("tp"), lax.axis_index("sp")
    side = jnp.where(me % 2 == line % 2, 1, -1)
    rows = block.shape[0]

    def owner(k):
        return (me + k * side + devices) % devices

    pair = jnp.concatenate([block, swapped(block, 0)], axis=0)
    blocks = [(owner(0), pair[:rows]), (owner(1), pair[rows:])]
    for step in range(1, devices // 2):
        pair = swapped(pair, step)
        near = -step if step % 2 else step
        far = near - 1 if step % 2 else near + 1
        blocks += [(owner(near), pair[:rows]), (owner(far), pair[rows:])]
    return blocks


def product(a, b):
    return jnp.dot(a, b, preferred_element_type=F32)


def through_kernel(rows, weight, own, out):
    @pl.when(pl.program_id(0) < 3)
    def _():
        out[0] = product(rows[...], weight[0]).astype(out.dtype)

    @pl.when(pl.program_id(0) == 3)
    def _():
        out[0] = own[...]


def through(rows, weights, own):
    count, depth = rows.shape
    width = own.shape[1]
    return pl.pallas_call(
        through_kernel,
        grid=(4,),
        out_shape=jax.ShapeDtypeStruct((4, count, width), BF16),
        in_specs=[
            pl.BlockSpec((count, depth), lambda j: (0, 0)),
            pl.BlockSpec((1, depth, width), lambda j: (jnp.minimum(2 * j + 1, 5), 0, 0)),
            pl.BlockSpec((count, width), lambda j: (0, 0)),
        ],
        out_specs=pl.BlockSpec((1, count, width), lambda j: (j, 0, 0)),
        cost_estimate=pl.CostEstimate(
            flops=6 * count * depth * width, bytes_accessed=6 * depth * width, transcendentals=0
        ),
    )(rows, weights, own)


def convolve(carried, tap_rows):
    reach = tap_rows.shape[0] - 1
    count = carried.shape[0]
    padded = jnp.concatenate([jnp.zeros((reach, carried.shape[1]), F32), carried], axis=0)
    result = jnp.zeros_like(carried)
    for tap in range(reach + 1):
        result = result + tap_rows[tap].astype(F32) * padded[tap : tap + count]
    return result


def gated(projected, tap_rows):
    gate, inner, values = (p.astype(BF16).astype(F32) for p in projected)
    return (gate * convolve(inner * values, tap_rows)).astype(BF16)


def factor_of(squares, count):
    return lax.rsqrt(squares / count + EPS)


def shards(tokens, mix_gain, gate_weight, mix_weight, value_weight, out_weight, conv_taps):
    _, _, width = gate_weight.shape
    features = mix_gain.shape[1]
    reach = conv_taps.shape[1] - 1
    fringe = -(-reach * 2 // TILE_ROWS) * TILE_ROWS
    inward = (gate_weight, mix_weight, value_weight)
    mine = jnp.concatenate([*inward, out_weight[:1]], axis=0)
    early = lax.all_gather(mine, "sp", axis=1, tiled=True)

    before = passed_along(tokens[tokens.shape[0] - fringe :], "sp", 1)
    stream = jnp.concatenate([before, tokens], axis=0)
    whole = whole_rows(stream, "tp").astype(F32)
    factor = factor_of(jnp.sum(whole * whole, axis=1, keepdims=True), features)
    normed = (whole * factor * mix_gain[0].astype(F32)).astype(BF16)
    scaled = (whole * mix_gain[1].astype(F32)).astype(BF16)

    shared = side_by_side(out_weight[0], "tp")
    shared, normed, scaled = lax.optimization_barrier((shared, normed, scaled))
    out_rows = (shared.astype(F32) * mix_gain[1].astype(F32)).astype(BF16)
    late = lax.all_gather(through(out_rows, early, out_weight[1]), "sp", axis=1, tiled=True)

    mixed = gated([product(normed, early[2 * k]) for k in range(3)], conv_taps[0])
    straight = [product(scaled, early[2 * k + 1]) for k in range(3)]
    all_mixed, *straight = lax.optimization_barrier((whole_rows(mixed, "tp"), *straight))
    stream = (stream.astype(F32) + product(all_mixed, early[6])).astype(BF16)
    wide = stream.astype(F32)
    squares = summed(jnp.sum(wide * wide, axis=1), "tp")
    factor = factor_of(squares, features)[:, None]

    mixed = gated([(straight[k] + product(all_mixed, late[k])) * factor for k in range(3)], conv_taps[1])
    results = []
    count = tokens.shape[0] // CHUNKS
    for c in range(CHUNKS):
        part = slice(fringe + c * count, fringe + (c + 1) * count)
        total = stream[part].astype(F32)
        for owner, block in arriving(mixed[part]):
            total = total + product(block, lax.dynamic_slice_in_dim(late[3], owner * width, width, axis=0))
        results.append(total.astype(BF16))
    return jnp.concatenate(results, axis=0)


def solution(mesh):
    return jax.shard_map(
        shards,
        mesh=mesh,
        in_specs=(
            P(("grp", "sp"), "tp"),
            P(),
            P(None, "sp", "tp"),
            P(None, "sp", "tp"),
            P(None, "sp", "tp"),
            P(None, "sp", "tp"),
            P(None, None, "tp"),
        ),
        out_specs=P(("grp", "sp"), "tp"),
        check_vma=False,
    )
```
